32 devices in a mesh: sp: 16 (over z, y, x), tp: 2 (over core).
Axes of the slice: x: 2, y: 2, z: 4, core: 2. Of those that a mesh axis runs over, the one named last changes fastest.
Arguments:
- tokens: bfloat16 [16384, 2048], P('sp', 'tp'), may hold values from -6 to 6
- norm_gain: float32 [2048], replicated, may hold values from 0.1 to 1.9
- w_conv_a: bfloat16 [2048, 1024], P('sp', 'tp'), may hold values from -0.125 to 0.125
- w_conv_gate: bfloat16 [2048, 1024], P('sp', 'tp'), may hold values from -0.125 to 0.125
- conv_weight: float32 [31, 1024], P(None, 'tp'), may hold values from -16 to 16
- conv_gain: float32 [1024], P('tp'), may hold values from 0.1 to 1.9
- w_query: bfloat16 [2048, 512], P('sp', 'tp'), may hold values from -0.125 to 0.125
- w_key: bfloat16 [2048, 512], P('sp', 'tp'), may hold values from -0.125 to 0.125
- w_value: bfloat16 [2048, 1024], P('sp', 'tp'), may hold values from -0.125 to 0.125
- w_outgate: bfloat16 [2048, 1024], P('sp', 'tp'), may hold values from -0.125 to 0.125
- w_decay: bfloat16 [2048, 512], P('sp', 'tp'), may hold values from -0.125 to 0.125
- decay_bias: float32 [512], P('tp'), may hold values from 0 to 12
- decay_extra: float32 [16384, 512], P('sp', 'tp'), may hold values from -2 to 0
- head_gain: float32 [128], replicated, may hold values from 0.1 to 1.9
- init_state: float32 [8, 64, 128], P('tp'), may hold values from -768 to 768
- w_out_conv: bfloat16 [1024, 2048], P('tp', 'sp'), may hold values from -0.125 to 0.125
- w_out_gla: bfloat16 [1024, 2048], P('tp', 'sp'), may hold values from -0.125 to 0.125
Outputs:
- mixed: bfloat16 [16384, 2048], P(('sp', 'tp'))
The draws below stay inside these ranges and needn't reach their ends.
All inputs are finite; a program needn't handle non-finite values.
Results may differ from the reference program's by a relative error of at most 0.022.
Values may be sent and summed in bfloat16 or wider, within the bound.
A program may use at most 128 MiB of HBM per device.

```python
import jax
import jax.numpy as jnp
from jax import lax

D = 2048
D_CONV = 1024
HEADS = 8
HK = 64
HV = 128
KERNEL = 31
BLOCK = 64
TOK_DEV = 1024
SEQUENCE_TOKENS = 16384
GLA_K = 512
GLA_V = 1024
N_TP = 2


def draw_conv_weight(key, part):
    key_base = jax.random.fold_in(key, 0)
    base = jax.random.normal(key_base, (KERNEL, D_CONV), jnp.float32) * KERNEL ** (-0.5)
    rising = 3.0 ** (jnp.arange(D_CONV, dtype=jnp.float32) / (D_CONV - 1))
    return base * rising[None, :]


def draw_decay_bias(key, part):
    key_pick, key_fast, key_slow = jax.random.split(key, 3)
    fast_share = 0.5
    fast_head = jax.random.bernoulli(key_pick, fast_share, (HEADS,))
    fast_values = jax.random.uniform(key_fast, (HEADS, HK), jnp.float32, 0.0, 1.0)
    slow_values = jax.random.uniform(key_slow, (HEADS, HK), jnp.float32, 8.0, 12.0)
    return jnp.where(fast_head[:, None], fast_values, slow_values).reshape(HEADS * HK)


def draw_decay_extra(key, part):
    key_factor, key_location, key_width, key_channel = jax.random.split(key, 4)
    factor = jax.random.uniform(key_factor, (SEQUENCE_TOKENS // TOK_DEV, 1), jnp.float32, 1.0, 3.0)
    row_each = jnp.repeat(factor, TOK_DEV, axis=0)
    channel_index = jax.random.uniform(key_channel, (1, HEADS * HK), jnp.float32, 0.5, 1.5)
    spike_locations = jax.random.randint(key_location, (3,), 0, SEQUENCE_TOKENS)
    spike_depth = jax.random.uniform(key_width, (3, 1), jnp.float32, 0.22, 0.5)
    spike_events = (jnp.arange(SEQUENCE_TOKENS)[:, None] == spike_locations[None, :]).astype(jnp.float32)
    return -(0.4 / SEQUENCE_TOKENS) * row_each * channel_index - jnp.dot(spike_events, spike_depth)


def block_scale(rng, extent, cuts, least, high):
    def one(dim, shards_of):
        steps = jax.random.uniform(jax.random.fold_in(jax.random.fold_in(rng, 6), dim), (shards_of,), jnp.float32, least / len(cuts), high / len(cuts))
        return jnp.repeat(jnp.exp(steps), extent[dim] // shards_of).reshape((-1,) + (1,) * (len(extent) - dim - 1))

    factor_of = one(*cuts[0])
    for cut in cuts[1:]:
        factor_of = factor_of * one(*cut)
    return factor_of


def bell_draw(key, shape, scale, most, shards=(), kind=jnp.bfloat16):
    entries = jax.random.normal(key, shape, jnp.float32) * scale
    if len(shards) > 0:
        entries = block_scale(key, shape, shards, -0.22, 0.18) * entries
    return jnp.clip(entries, min=-most, max=most).astype(kind)


def setup_inputs(seed: int = 0) -> dict:
    streams_of = jax.random.split(jax.random.key(seed), 18)
    return {
        "tokens": bell_draw(streams_of[0], (SEQUENCE_TOKENS, D), 1.0, 6.0, ((0, 16), (1, 2))),
        "norm_gain": jnp.clip(1.0 + 0.18 * jax.random.normal(streams_of[1], (D,), jnp.float32), 0.1, 1.9),
        "w_conv_a": bell_draw(streams_of[2], (D, D_CONV), D ** -0.5, 0.125, ((0, 16), (1, 2))),
        "w_conv_gate": bell_draw(streams_of[3], (D, D_CONV), D ** -0.5, 0.125, ((0, 16), (1, 2))),
        "conv_weight": draw_conv_weight(jax.random.fold_in(streams_of[17], 71), 0),
        "conv_gain": jnp.clip(1.0 + 0.18 * jax.random.normal(streams_of[5], (D_CONV,), jnp.float32), 0.1, 1.9),
        "w_query": bell_draw(streams_of[6], (D, GLA_K), D ** -0.5, 0.125, ((0, 16), (1, 2))),
        "w_key": bell_draw(streams_of[7], (D, GLA_K), D ** -0.5, 0.125, ((0, 16), (1, 2))),
        "w_value": bell_draw(streams_of[8], (D, GLA_V), D ** -0.5, 0.125, ((0, 16), (1, 2))),
        "w_outgate": bell_draw(streams_of[9], (D, GLA_V), D ** -0.5, 0.125, ((0, 16), (1, 2))),
        "w_decay": bell_draw(streams_of[10], (D, GLA_K), D ** -0.5, 0.125, ((0, 16), (1, 2))),
        "decay_bias": draw_decay_bias(jax.random.fold_in(streams_of[17], 71), 0),
        "decay_extra": draw_decay_extra(jax.random.fold_in(streams_of[17], 71), 0),
        "head_gain": jnp.clip(1.0 + 0.18 * jax.random.normal(streams_of[13], (HV,), jnp.float32), 0.1, 1.9),
        "init_state": bell_draw(streams_of[14], (HEADS, HK, HV), (SEQUENCE_TOKENS ** 0.5), 768.0, ((0, 2),), jnp.float32),
        "w_out_conv": bell_draw(streams_of[15], (D_CONV, D), (D_CONV + GLA_V) ** -0.5, 0.125, ((0, 2), (1, 16))),
        "w_out_gla": bell_draw(streams_of[16], (GLA_V, D), (D_CONV + GLA_V) ** -0.5, 0.125, ((0, 2), (1, 16))),
    }


epsilon = 1e-06
gate_divisor = 16.0
highest_precision = lax.Precision.HIGHEST

def project(hidden, weight):
    return jnp.dot(hidden, weight, preferred_element_type=jnp.float32)

def rounded(values_f32):
    return lax.optimization_barrier(values_f32.astype(jnp.bfloat16)).astype(jnp.float32)

def reference(tokens, norm_gain, w_conv_a, w_conv_gate, conv_weight, conv_gain, w_query, w_key, w_value, w_outgate, w_decay, decay_bias, decay_extra, head_gain, init_state, w_out_conv, w_out_gla):
    widened = tokens.astype(jnp.float32)
    normed = (widened * lax.rsqrt(lax.optimization_barrier(jnp.mean(widened * widened, axis=-1, keepdims=True)) + epsilon) * norm_gain).astype(jnp.bfloat16)
    conv_a = rounded(project(normed, w_conv_a))
    conv_gate = rounded(project(normed, w_conv_gate))
    query = rounded(project(normed, w_query))
    keys = rounded(project(normed, w_key))
    values = rounded(project(normed, w_value))
    out_gate = rounded(project(normed, w_outgate))
    decay_pre = project(normed, w_decay)
    gated = rounded(conv_a * jax.nn.sigmoid(conv_gate))
    padded = jnp.pad(gated, ((KERNEL - 1, 0), (0, 0)))
    conv_sum = jnp.zeros((SEQUENCE_TOKENS, D_CONV), jnp.float32)
    for tap_index in range(KERNEL):
        conv_sum = conv_sum + conv_weight[tap_index][None, :] * padded[tap_index:tap_index + SEQUENCE_TOKENS]
    mean_val = lax.optimization_barrier(jnp.mean(conv_sum, axis=-1, keepdims=True))
    square_mean = lax.optimization_barrier(jnp.mean(conv_sum * conv_sum, axis=-1, keepdims=True))
    conv_norm = (conv_sum - mean_val) * lax.rsqrt(square_mean - mean_val * mean_val + epsilon) * conv_gain
    conv_out = jax.nn.silu(conv_norm).astype(jnp.bfloat16)
    log_decay = jax.nn.log_sigmoid(decay_pre + decay_bias) / gate_divisor + decay_extra
    blocks = SEQUENCE_TOKENS // BLOCK

    def to_heads(array, width):
        return array.astype(jnp.float32).reshape(blocks, BLOCK, HEADS, width).transpose(0, 2, 1, 3)
    query_heads = to_heads(query, HK) * HK ** (-0.5)
    key_heads = to_heads(keys, HK)
    value_heads = to_heads(values, HV)
    cum_log = jnp.cumsum(to_heads(log_decay, HK), axis=2)
    block_total = cum_log[:, :, -1:, :]
    query_decayed = query_heads * jnp.exp(cum_log)
    key_inverse = key_heads * jnp.exp(-cum_log)
    key_to_end = key_heads * jnp.exp(block_total - cum_log)
    causal = jnp.tril(jnp.ones((BLOCK, BLOCK), dtype=bool))
    scores = jnp.where(causal, jnp.einsum('nhik,nhjk->nhij', query_decayed, key_inverse, precision=highest_precision), 0.0)
    within = jnp.einsum('nhij,nhjv->nhiv', scores, value_heads, precision=highest_precision)

    def advance(state_current, block_items):
        query_block, key_block, value_block, decay_block = block_items
        carried_state = jnp.einsum('yau,yub->yab', query_block, state_current, precision=highest_precision)
        state_following = state_current * decay_block[:, 0, :, None] + jnp.einsum('tie,tis->tes', key_block, value_block, precision=highest_precision)
        return (state_following, carried_state)
    final_state, carried_out = lax.scan(advance, init_state.astype(jnp.float32), (query_decayed, key_to_end, value_heads, jnp.exp(block_total)))
    attn = within + carried_out
    normal_attn = attn * lax.rsqrt(lax.optimization_barrier(jnp.mean(attn * attn, axis=-1, keepdims=True)) + epsilon) * head_gain
    normal_attn = normal_attn.transpose(0, 2, 1, 3).reshape(SEQUENCE_TOKENS, HEADS * HV)
    gla_out = (normal_attn * jax.nn.silu(out_gate)).astype(jnp.bfloat16)
    conv_share = D_CONV // N_TP
    value_share = HEADS * HV // N_TP
    totals = jnp.zeros((SEQUENCE_TOKENS, D), jnp.float32)
    for group_index in range(N_TP):
        partial_value = project(conv_out[:, group_index * conv_share:(group_index + 1) * conv_share], w_out_conv[group_index * conv_share:(group_index + 1) * conv_share])
        partial_value = partial_value + project(gla_out[:, group_index * value_share:(group_index + 1) * value_share], w_out_gla[group_index * value_share:(group_index + 1) * value_share])
        totals = totals + rounded(partial_value)
    return totals.astype(jnp.bfloat16)
```

```python
import functools

import jax
import jax.numpy as jnp
from jax import lax
from jax.experimental import pallas as pl
from jax.experimental.pallas import tpu as pltpu
from jax.sharding import PartitionSpec as P

D_CONV = 1024
HK = 64
HV = 128
BLOCK = 64

epsilon = 1e-06
gate_divisor = 16.0


def dot(a, b, dims):
    return lax.dot_general(a, b, (dims, ((), ())), preferred_element_type=jnp.float32)


def folded(n_sp, n_tp):
    return n_sp == 16 and n_tp == 2


def exchange(array, mask):
    count = lax.axis_size("sp")
    return lax.ppermute(array, "sp", [(i, i ^ mask) for i in range(count)])


def gather_rows(shard, x_last):
    part = jnp.concatenate(
        [shard, exchange(shard, 4), exchange(shard, 8), exchange(shard, 12)], axis=0
    )
    if x_last:
        part = jnp.concatenate([part, exchange(part, 2)], axis=0)
        return jnp.concatenate([part, exchange(part, 1)], axis=0)
    rows = part.shape[0]
    far = exchange(part, 1)
    part = jnp.concatenate([part, far], axis=0)
    other = exchange(part, 2)
    return jnp.concatenate([part[:rows], other[:rows], part[rows:], other[rows:]], axis=0)


def relative(place, me):
    z = place % 4
    y = (place // 4) % 2
    x = place // 8
    return me ^ (z * 4 + y * 2 + x)


def place_of(device, me):
    step = device ^ me
    return (step & 1) * 8 + ((step >> 1) & 1) * 4 + (step >> 2)


def norm_kernel(blocks, where_ref, own_ref, other_ref, gain_ref, out_ref):
    me, tp = where_ref[0], where_ref[1]
    own = own_ref[...].astype(jnp.float32)
    other = other_ref[...].astype(jnp.float32)
    width = own.shape[1] * 2
    square = jnp.sum(own * own, axis=1, keepdims=True) + jnp.sum(other * other, axis=1, keepdims=True)
    scale = lax.rsqrt(square / width + epsilon)
    size = width // blocks
    half = blocks // 2
    for place in range(blocks):
        block = relative(place, me)
        inner = pl.ds(pl.multiple_of((block % half) * size, size), size)
        gain = gain_ref[:, pl.ds(pl.multiple_of(block * size, size), size)]
        mine = (block // half) == tp
        value = jnp.where(mine, own_ref[:, inner].astype(jnp.float32), other_ref[:, inner].astype(jnp.float32))
        out_ref[:, place * size : (place + 1) * size] = (value * scale * gain).astype(jnp.bfloat16)


def norm_folded(tokens, gain, me, tp):
    rows, half = tokens.shape
    other = lax.ppermute(tokens, "tp", [(0, 1), (1, 0)])
    tile = 256
    spec = pl.BlockSpec((tile, half), lambda i, w: (i, 0))
    return pl.pallas_call(
        functools.partial(norm_kernel, lax.axis_size("sp")),
        grid_spec=pltpu.PrefetchScalarGridSpec(
            num_scalar_prefetch=1,
            grid=(rows // tile,),
            in_specs=[spec, spec, pl.BlockSpec((1, 2 * half), lambda i, w: (0, 0))],
            out_specs=pl.BlockSpec((tile, 2 * half), lambda i, w: (i, 0)),
        ),
        out_shape=jax.ShapeDtypeStruct((rows, 2 * half), jnp.bfloat16),
        cost_estimate=pl.CostEstimate(flops=rows * half * 8, bytes_accessed=rows * half * 8, transcendentals=0),
        name="norm",
    )(jnp.stack([me, tp]), tokens, other, gain[None, :])


def local_kernel(heads, pieces, q_ref, k_ref, v_ref, pre_ref, extra_ref, bias_ref, attn_ref, since_ref, end_ref, log_ref, state, prefix):
    step = pl.program_id(0)

    @pl.when(step == 0)
    def _():
        state[...] = jnp.zeros_like(state)
        prefix[...] = jnp.zeros_like(prefix)

    rows = lax.broadcasted_iota(jnp.int32, (BLOCK, BLOCK), 0)
    columns = lax.broadcasted_iota(jnp.int32, (BLOCK, BLOCK), 1)
    causal = rows >= columns
    lower = causal.astype(jnp.float32)
    for piece in range(pieces):
        at = pl.ds(piece * BLOCK, BLOCK)
        pre = pre_ref[at, :] + bias_ref[...]
        logs = jax.nn.log_sigmoid(pre) / gate_divisor + extra_ref[at, :]
        cum = lax.dot_general(
            lower, logs, (((1,), (0,)), ((), ())), precision=lax.Precision.HIGHEST, preferred_element_type=jnp.float32
        )
        total = cum[BLOCK - 1 :, :]
        middle = cum[BLOCK // 2 - 1 : BLOCK // 2, :]
        query = q_ref[at, :].astype(jnp.float32) * HK ** (-0.5)
        keys = k_ref[at, :].astype(jnp.float32)
        decayed = query * jnp.exp(cum)
        since_ref[at, :] = (decayed * jnp.exp(prefix[...])).astype(jnp.bfloat16)
        decayed = decayed.astype(jnp.bfloat16)
        query = (query * jnp.exp(cum - middle)).astype(jnp.bfloat16)
        inverse = (keys * jnp.exp(middle - cum)).astype(jnp.bfloat16)
        to_end = (keys * jnp.exp(total - cum)).astype(jnp.bfloat16)
        entering = state[...].astype(jnp.bfloat16)
        added = []
        for h in range(heads):
            ks, vs = slice(h * HK, (h + 1) * HK), slice(h * HV, (h + 1) * HV)
            values = v_ref[at, vs]
            scores = jnp.where(causal, dot(query[:, ks], inverse[:, ks], ((1,), (1,))), 0.0)
            attn_ref[at, vs] = dot(scores.astype(jnp.bfloat16), values, ((1,), (0,))) + dot(
                decayed[:, ks], entering[:, ks], ((1,), (1,))
            )
            added.append(dot(values, to_end[:, ks], ((0,), (0,))))
        added = added[0] if heads == 1 else jnp.concatenate(added, axis=1)
        state[...] = state[...] * jnp.exp(total) + added
        prefix[...] = prefix[...] + total
    end_ref[...] = state[...]
    log_ref[...] = prefix[...]


def gla_local(query, keys, values, decay_pre, decay_extra, decay_bias):
    rows, width = query.shape
    heads = width // HK
    pieces = 4
    tile = pieces * BLOCK

    def tiled(array):
        return pl.BlockSpec((tile, array.shape[1]), lambda i: (i, 0))

    def whole(shape):
        return pl.BlockSpec(shape, lambda i: (0, 0))

    return pl.pallas_call(
        functools.partial(local_kernel, heads, pieces),
        grid=(rows // tile,),
        in_specs=[tiled(query), tiled(keys), tiled(values), tiled(decay_pre), tiled(decay_extra), whole((1, width))],
        out_specs=[tiled(values), tiled(query), whole((HV, width)), whole((1, width))],
        out_shape=[
            jax.ShapeDtypeStruct(values.shape, jnp.float32),
            jax.ShapeDtypeStruct(query.shape, jnp.bfloat16),
            jax.ShapeDtypeStruct((HV, width), jnp.float32),
            jax.ShapeDtypeStruct((1, width), jnp.float32),
        ],
        scratch_shapes=[pltpu.VMEM((HV, width), jnp.float32), pltpu.VMEM((1, width), jnp.float32)],
        cost_estimate=pl.CostEstimate(flops=10**10, bytes_accessed=10**7, transcendentals=10**6),
        name="gla_local",
    )(query, keys, values, decay_pre, decay_extra, decay_bias[None, :])


def finish_kernel(heads, size, fold, where_ref, attn_ref, since_ref, gate_ref, ends_ref, init_ref, gain_ref, out_ref, state):
    me = where_ref[0]

    @pl.when(pl.program_id(0) == 0)
    def _():
        state[...] = init_ref[...]

        def one(device, carry):
            at = place_of(device, me) if fold else device
            decay = ends_ref[pl.ds(pl.multiple_of(at * size + HV, 16), 16), :].astype(jnp.float32)[:1]
            end = ends_ref[pl.ds(pl.multiple_of(at * size, 16), HV), :].astype(jnp.float32)
            state[...] = state[...] * decay + end
            return carry

        lax.fori_loop(0, me, one, 0)

    entering = state[...].astype(jnp.bfloat16)
    for h in range(heads):
        ks, vs = slice(h * HK, (h + 1) * HK), slice(h * HV, (h + 1) * HV)
        attn = attn_ref[:, vs] + dot(since_ref[:, ks], entering[:, ks], ((1,), (1,)))
        attn = attn * lax.rsqrt(jnp.mean(attn * attn, axis=-1, keepdims=True) + epsilon) * gain_ref[...]
        gate = gate_ref[:, vs].astype(jnp.float32)
        out_ref[:, vs] = (attn * (gate * jax.nn.sigmoid(gate))).astype(jnp.bfloat16)


def gla_finish(attn, since, out_gate, ends, init_state, head_gain, me, fold):
    rows, width = since.shape
    heads = width // HK
    tile = 256

    def tiled(array):
        return pl.BlockSpec((tile, array.shape[1]), lambda i, w: (i, 0))

    def whole(array):
        return pl.BlockSpec(array.shape, lambda i, w: (0, 0))

    init = init_state.transpose(2, 0, 1).reshape(HV, width)
    gain = head_gain[None, :]
    return pl.pallas_call(
        functools.partial(finish_kernel, heads, HV + 16, fold),
        grid_spec=pltpu.PrefetchScalarGridSpec(
            num_scalar_prefetch=1,
            grid=(rows // tile,),
            in_specs=[tiled(attn), tiled(since), tiled(out_gate), whole(ends), whole(init), whole(gain)],
            out_specs=tiled(attn),
            scratch_shapes=[pltpu.VMEM((HV, width), jnp.float32)],
        ),
        out_shape=jax.ShapeDtypeStruct(attn.shape, jnp.bfloat16),
        cost_estimate=pl.CostEstimate(flops=3 * 10**9, bytes_accessed=10**7, transcendentals=10**6),
        name="gla_finish",
    )(me[None], attn, since, out_gate, ends, init, gain)


def merge_kernel(blocks, where_ref, own_ref, other_ref, out_ref):
    me = where_ref[0]
    size = own_ref.shape[1] // blocks
    for place in range(blocks):
        at = slice(place * size, (place + 1) * size)
        target = pl.ds(pl.multiple_of(relative(place, me) * size, size), size)
        total = own_ref[:, at].astype(jnp.float32) + other_ref[:, at].astype(jnp.float32)
        out_ref[:, target] = total.astype(jnp.bfloat16)


def merge_folded(own, other, me):
    rows, width = own.shape
    tile = 128
    spec = pl.BlockSpec((tile, width), lambda i, w: (i, 0))
    return pl.pallas_call(
        functools.partial(merge_kernel, lax.axis_size("sp")),
        grid_spec=pltpu.PrefetchScalarGridSpec(
            num_scalar_prefetch=1, grid=(rows // tile,), in_specs=[spec, spec], out_specs=spec
        ),
        out_shape=jax.ShapeDtypeStruct((rows, width), jnp.bfloat16),
        name="merge",
    )(me[None], own, other)


def conv_branch(conv_a, conv_gate, conv_weight, conv_gain):
    gated = (conv_a.astype(jnp.float32) * jax.nn.sigmoid(conv_gate.astype(jnp.float32))).astype(jnp.bfloat16)
    taps = conv_weight.shape[0]
    row_count = gated.shape[0]
    count = lax.axis_size("sp")
    earlier = lax.ppermute(gated[row_count - taps + 1 :], "sp", [(i, i + 1) for i in range(count - 1)])
    extended = jnp.concatenate([earlier, gated], axis=0).astype(jnp.float32)
    conv_sum = jnp.zeros(gated.shape, jnp.float32)
    for tap in range(taps):
        conv_sum = conv_sum + conv_weight[tap][None, :] * extended[tap : tap + row_count]
    row_sums, row_squares = lax.psum((jnp.sum(conv_sum, axis=1), jnp.sum(conv_sum * conv_sum, axis=1)), "tp")
    mean_val = (row_sums / D_CONV)[:, None]
    square_mean = (row_squares / D_CONV)[:, None]
    conv_norm = (conv_sum - mean_val) * lax.rsqrt(square_mean - mean_val * mean_val + epsilon) * conv_gain
    return jax.nn.silu(conv_norm).astype(jnp.bfloat16)


def project(hidden, weight):
    return dot(hidden, weight, ((1,), (0,)))


def per_device(
    tokens, norm_gain, w_conv_a, w_conv_gate, conv_weight, conv_gain, w_query, w_key, w_value, w_outgate,
    w_decay, decay_bias, decay_extra, head_gain, init_state, w_out_conv, w_out_gla,
):
    n_sp, n_tp = lax.axis_size("sp"), lax.axis_size("tp")
    fold = folded(n_sp, n_tp)
    me = lax.axis_index("sp")
    tp = lax.axis_index("tp")
    if fold:
        gather = gather_rows
        normed = norm_folded(tokens, norm_gain, me, tp)
    else:

        def gather(shard, x_last):
            return lax.all_gather(shard, "sp", axis=0, tiled=True)

        widened = lax.all_gather(tokens, "tp", axis=1, tiled=True).astype(jnp.float32)
        normed = (
            widened * lax.rsqrt(jnp.mean(widened * widened, axis=-1, keepdims=True) + epsilon) * norm_gain
        ).astype(jnp.bfloat16)

    half = w_query.shape[1]
    conv_a = project(normed, gather(w_conv_a, True)).astype(jnp.bfloat16)
    conv_gate = project(normed, gather(w_conv_gate, False)).astype(jnp.bfloat16)
    query_keys = project(normed, gather(jnp.concatenate([w_query, w_key], axis=1), True)).astype(jnp.bfloat16)
    values = project(normed, gather(w_value, False)).astype(jnp.bfloat16)
    decay_pre = project(normed, gather(w_decay, True))
    out_gate = project(normed, gather(w_outgate, False)).astype(jnp.bfloat16)
    out_conv = gather(w_out_conv.T, True)
    out_gla = gather(w_out_gla.T, False)

    conv_out = conv_branch(conv_a, conv_gate, conv_weight, conv_gain)

    attn, since, end, end_log = gla_local(
        query_keys[:, :half], query_keys[:, half:], values, decay_pre, decay_extra, decay_bias
    )
    packed = jnp.concatenate([end, jnp.broadcast_to(jnp.exp(end_log), (16, half))], axis=0).astype(jnp.bfloat16)
    ends = gather(packed, True)
    gla_out = gla_finish(attn, since, out_gate, ends, init_state, head_gain, me, fold)

    def merged(conv_rows, gla_rows):
        total = dot(conv_rows, out_conv, ((1,), (1,))) + dot(gla_rows, out_gla, ((1,), (1,)))
        return total.astype(jnp.bfloat16)

    if not fold:
        return lax.psum_scatter(merged(conv_out, gla_out), "tp", scatter_dimension=0, tiled=True)
    rows = conv_out.shape[0] // 2

    def part(index):
        return merged(
            lax.dynamic_slice_in_dim(conv_out, index * rows, rows),
            lax.dynamic_slice_in_dim(gla_out, index * rows, rows),
        )

    arriving = lax.ppermute(part(1 - tp), "tp", [(0, 1), (1, 0)])
    return merge_folded(part(tp), arriving, me)


def solution(mesh):
    placed = (
        P("sp", "tp"), P(), P("sp", "tp"), P("sp", "tp"), P(None, "tp"), P("tp"), P("sp", "tp"), P("sp", "tp"),
        P("sp", "tp"), P("sp", "tp"), P("sp", "tp"), P("tp"), P("sp", "tp"), P(), P("tp", None, None),
        P("tp", "sp"), P("tp", "sp"),
    )
    return jax.shard_map(
        per_device, mesh=mesh, in_specs=placed, out_specs=P(("sp", "tp"), None), check_vma=False
    )
```

```python
import functools

import jax
import jax.numpy as jnp
from jax import lax
from jax.experimental import pallas as pl
from jax.experimental.pallas import tpu as pltpu
from jax.sharding import PartitionSpec as P


D_CONV = 1024
HK = 64
HV = 128
BLOCK = 64

epsilon = 1e-06
gate_divisor = 16.0


def dot(a, b, dims):
    return lax.dot_general(a, b, (dims, ((), ())), preferred_element_type=jnp.float32)


def folded(n_sp, n_tp):
    return n_sp == 16 and n_tp == 2


def exchange(array, mask):
    count = lax.axis_size("sp")
    return lax.ppermute(array, "sp", [(i, i ^ mask) for i in range(count)])


def along_z(shard):
    return jnp.concatenate(
        [shard, exchange(shard, 4), exchange(shard, 8), exchange(shard, 12)], axis=0
    )


def finish_x(near):
    return jnp.concatenate([near, exchange(near, 1)], axis=0)


def finish_y(near):
    rows = near.shape[0] // 2
    far = exchange(near, 2)
    return jnp.concatenate([near[:rows], far[:rows], near[rows:], far[rows:]], axis=0)


def after(arrays, *earlier):
    count = len(arrays)
    return lax.optimization_barrier((*arrays, *earlier))[:count]


def gather_rows(shard):
    part = along_z(shard)
    return finish_x(jnp.concatenate([part, exchange(part, 2)], axis=0))


def along_z_pair(first, second):
    part = along_z(jnp.concatenate([first, second], axis=1))
    return part[:, : first.shape[1]], part[:, first.shape[1] :]


def near_pair(first, second):
    return (
        jnp.concatenate([first, exchange(first, 2)], axis=0),
        jnp.concatenate([second, exchange(second, 1)], axis=0),
    )


def far_pair(first, second):
    return finish_x(first), finish_y(second)


def relative(place, me):
    z = place % 4
    y = (place // 4) % 2
    x = place // 8
    return me ^ (z * 4 + y * 2 + x)


def place_of(device, me):
    step = device ^ me
    return (step & 1) * 8 + ((step >> 1) & 1) * 4 + (step >> 2)


def norm_kernel(blocks, where_ref, own_ref, other_ref, gain_ref, out_ref):
    me, tp = where_ref[0], where_ref[1]
    own = own_ref[...].astype(jnp.float32)
    other = other_ref[...].astype(jnp.float32)
    width = own.shape[1] * 2
    square = jnp.sum(own * own, axis=1, keepdims=True) + jnp.sum(other * other, axis=1, keepdims=True)
    scale = lax.rsqrt(square / width + epsilon)
    size = width // blocks
    half = blocks // 2
    for place in range(blocks):
        block = relative(place, me)
        inner = pl.ds(pl.multiple_of((block % half) * size, size), size)
        gain = gain_ref[:, pl.ds(pl.multiple_of(block * size, size), size)]
        mine = (block // half) == tp
        value = jnp.where(mine, own_ref[:, inner].astype(jnp.float32), other_ref[:, inner].astype(jnp.float32))
        out_ref[:, place * size : (place + 1) * size] = (value * scale * gain).astype(jnp.bfloat16)


def norm_folded(tokens, gain, me, tp):
    rows, half = tokens.shape
    other = lax.ppermute(tokens, "tp", [(0, 1), (1, 0)])
    tile = 256
    spec = pl.BlockSpec((tile, half), lambda i, w: (i, 0))
    return pl.pallas_call(
        functools.partial(norm_kernel, lax.axis_size("sp")),
        grid_spec=pltpu.PrefetchScalarGridSpec(
            num_scalar_prefetch=1,
            grid=(rows // tile,),
            in_specs=[spec, spec, pl.BlockSpec((1, 2 * half), lambda i, w: (0, 0))],
            out_specs=pl.BlockSpec((tile, 2 * half), lambda i, w: (i, 0)),
        ),
        out_shape=jax.ShapeDtypeStruct((rows, 2 * half), jnp.bfloat16),
        cost_estimate=pl.CostEstimate(flops=rows * half * 8, bytes_accessed=rows * half * 8, transcendentals=0),
        name="norm",
    )(jnp.stack([me, tp]), tokens, other, gain[None, :])


def local_kernel(heads, pieces, q_ref, k_ref, v_ref, pre_ref, extra_ref, bias_ref, attn_ref, since_ref, end_ref, log_ref, state, prefix):
    step = pl.program_id(0)

    @pl.when(step == 0)
    def _():
        state[...] = jnp.zeros_like(state)
        prefix[...] = jnp.zeros_like(prefix)

    rows = lax.broadcasted_iota(jnp.int32, (BLOCK, BLOCK), 0)
    columns = lax.broadcasted_iota(jnp.int32, (BLOCK, BLOCK), 1)
    causal = rows >= columns
    lower = causal.astype(jnp.float32)
    for piece in range(pieces):
        at = pl.ds(piece * BLOCK, BLOCK)
        pre = pre_ref[at, :] + bias_ref[...]
        logs = jax.nn.log_sigmoid(pre) / gate_divisor + extra_ref[at, :]
        cum = lax.dot_general(
            lower, logs, (((1,), (0,)), ((), ())), precision=lax.Precision.HIGHEST, preferred_element_type=jnp.float32
        )
        total = cum[BLOCK - 1 :, :]
        middle = cum[BLOCK // 2 - 1 : BLOCK // 2, :]
        query = q_ref[at, :].astype(jnp.float32) * HK ** (-0.5)
        keys = k_ref[at, :].astype(jnp.float32)
        decayed = query * jnp.exp(cum)
        since_ref[at, :] = (decayed * jnp.exp(prefix[...])).astype(jnp.bfloat16)
        decayed = decayed.astype(jnp.bfloat16)
        query = (query * jnp.exp(cum - middle)).astype(jnp.bfloat16)
        inverse = (keys * jnp.exp(middle - cum)).astype(jnp.bfloat16)
        to_end = (keys * jnp.exp(total - cum)).astype(jnp.bfloat16)
        entering = state[...].astype(jnp.bfloat16)
        added = []
        for h in range(heads):
            ks, vs = slice(h * HK, (h + 1) * HK), slice(h * HV, (h + 1) * HV)
            values = v_ref[at, vs]
            scores = jnp.where(causal, dot(query[:, ks], inverse[:, ks], ((1,), (1,))), 0.0)
            attn_ref[at, vs] = dot(scores.astype(jnp.bfloat16), values, ((1,), (0,))) + dot(
                decayed[:, ks], entering[:, ks], ((1,), (1,))
            )
            added.append(dot(values, to_end[:, ks], ((0,), (0,))))
        added = added[0] if heads == 1 else jnp.concatenate(added, axis=1)
        state[...] = state[...] * jnp.exp(total) + added
        prefix[...] = prefix[...] + total
    end_ref[...] = state[...]
    log_ref[...] = prefix[...]


def gla_local(query, keys, values, decay_pre, decay_extra, decay_bias):
    rows, width = query.shape
    heads = width // HK
    pieces = 4
    tile = pieces * BLOCK

    def tiled(array):
        return pl.BlockSpec((tile, array.shape[1]), lambda i: (i, 0))

    def whole(shape):
        return pl.BlockSpec(shape, lambda i: (0, 0))

    return pl.pallas_call(
        functools.partial(local_kernel, heads, pieces),
        grid=(rows // tile,),
        in_specs=[tiled(query), tiled(keys), tiled(values), tiled(decay_pre), tiled(decay_extra), whole((1, width))],
        out_specs=[tiled(values), tiled(query), whole((HV, width)), whole((1, width))],
        out_shape=[
            jax.ShapeDtypeStruct(values.shape, jnp.float32),
            jax.ShapeDtypeStruct(query.shape, jnp.bfloat16),
            jax.ShapeDtypeStruct((HV, width), jnp.float32),
            jax.ShapeDtypeStruct((1, width), jnp.float32),
        ],
        scratch_shapes=[pltpu.VMEM((HV, width), jnp.float32), pltpu.VMEM((1, width), jnp.float32)],
        cost_estimate=pl.CostEstimate(flops=10**10, bytes_accessed=10**7, transcendentals=10**6),
        name="gla_local",
    )(query, keys, values, decay_pre, decay_extra, decay_bias[None, :])


def finish_kernel(heads, size, fold, where_ref, attn_ref, since_ref, gate_ref, ends_ref, init_ref, gain_ref, out_ref, state):
    me = where_ref[0]

    @pl.when(pl.program_id(0) == 0)
    def _():
        state[...] = init_ref[...]

        def one(device, carry):
            at = place_of(device, me) if fold else device
            decay = ends_ref[pl.ds(pl.multiple_of(at * size + HV, 16), 16), :].astype(jnp.float32)[:1]
            end = ends_ref[pl.ds(pl.multiple_of(at * size, 16), HV), :].astype(jnp.float32)
            state[...] = state[...] * decay + end
            return carry

        lax.fori_loop(0, me, one, 0)

    entering = state[...].astype(jnp.bfloat16)
    for h in range(heads):
        ks, vs = slice(h * HK, (h + 1) * HK), slice(h * HV, (h + 1) * HV)
        attn = attn_ref[:, vs] + dot(since_ref[:, ks], entering[:, ks], ((1,), (1,)))
        attn = attn * lax.rsqrt(jnp.mean(attn * attn, axis=-1, keepdims=True) + epsilon) * gain_ref[...]
        gate = gate_ref[:, vs].astype(jnp.float32)
        out_ref[:, vs] = (attn * (gate * jax.nn.sigmoid(gate))).astype(jnp.bfloat16)


def gla_finish(attn, since, out_gate, ends, init_state, head_gain, me, fold):
    rows, width = since.shape
    heads = width // HK
    tile = 256

    def tiled(array):
        return pl.BlockSpec((tile, array.shape[1]), lambda i, w: (i, 0))

    def whole(array):
        return pl.BlockSpec(array.shape, lambda i, w: (0, 0))

    init = init_state.transpose(2, 0, 1).reshape(HV, width)
    gain = head_gain[None, :]
    return pl.pallas_call(
        functools.partial(finish_kernel, heads, HV + 16, fold),
        grid_spec=pltpu.PrefetchScalarGridSpec(
            num_scalar_prefetch=1,
            grid=(rows // tile,),
            in_specs=[tiled(attn), tiled(since), tiled(out_gate), whole(ends), whole(init), whole(gain)],
            out_specs=tiled(attn),
            scratch_shapes=[pltpu.VMEM((HV, width), jnp.float32)],
        ),
        out_shape=jax.ShapeDtypeStruct(attn.shape, jnp.bfloat16),
        cost_estimate=pl.CostEstimate(flops=3 * 10**9, bytes_accessed=10**7, transcendentals=10**6),
        name="gla_finish",
    )(me[None], attn, since, out_gate, ends, init, gain)


def merge_kernel(blocks, where_ref, own_ref, other_ref, out_ref):
    me = where_ref[0]
    size = own_ref.shape[1] // blocks
    for place in range(blocks):
        at = slice(place * size, (place + 1) * size)
        target = pl.ds(pl.multiple_of(relative(place, me) * size, size), size)
        total = own_ref[:, at].astype(jnp.float32) + other_ref[:, at].astype(jnp.float32)
        out_ref[:, target] = total.astype(jnp.bfloat16)


def merge_folded(own, other, me):
    rows, width = own.shape
    tile = 128
    spec = pl.BlockSpec((tile, width), lambda i, w: (i, 0))
    return pl.pallas_call(
        functools.partial(merge_kernel, lax.axis_size("sp")),
        grid_spec=pltpu.PrefetchScalarGridSpec(
            num_scalar_prefetch=1, grid=(rows // tile,), in_specs=[spec, spec], out_specs=spec
        ),
        out_shape=jax.ShapeDtypeStruct((rows, width), jnp.bfloat16),
        name="merge",
    )(me[None], own, other)


def conv_branch(gated, conv_weight, conv_gain):
    taps = conv_weight.shape[0]
    row_count = gated.shape[0]
    count = lax.axis_size("sp")
    earlier = lax.ppermute(gated[row_count - taps + 1 :], "sp", [(i, i + 1) for i in range(count - 1)])
    extended = jnp.concatenate([earlier, gated], axis=0).astype(jnp.float32)
    conv_sum = jnp.zeros(gated.shape, jnp.float32)
    for tap in range(taps):
        conv_sum = conv_sum + conv_weight[tap][None, :] * extended[tap : tap + row_count]
    row_sums, row_squares = lax.psum((jnp.sum(conv_sum, axis=1), jnp.sum(conv_sum * conv_sum, axis=1)), "tp")
    mean_val = (row_sums / D_CONV)[:, None]
    square_mean = (row_squares / D_CONV)[:, None]
    conv_norm = (conv_sum - mean_val) * lax.rsqrt(square_mean - mean_val * mean_val + epsilon) * conv_gain
    return jax.nn.silu(conv_norm).astype(jnp.bfloat16)


def project(hidden, weight):
    return dot(hidden, weight, ((1,), (0,)))


def per_device(
    tokens, norm_gain, w_conv_a, w_conv_gate, conv_weight, conv_gain, w_query, w_key, w_value, w_outgate,
    w_decay, decay_bias, decay_extra, head_gain, init_state, w_out_conv, w_out_gla,
):
    n_sp, n_tp = lax.axis_size("sp"), lax.axis_size("tp")
    fold = folded(n_sp, n_tp)
    me = lax.axis_index("sp")
    tp = lax.axis_index("tp")
    if fold:
        gather = gather_rows
        normed = norm_folded(tokens, norm_gain, me, tp)
    else:

        def gather(shard):
            return lax.all_gather(shard, "sp", axis=0, tiled=True)

        widened = lax.all_gather(tokens, "tp", axis=1, tiled=True).astype(jnp.float32)
        normed = (
            widened * lax.rsqrt(jnp.mean(widened * widened, axis=-1, keepdims=True) + epsilon) * norm_gain
        ).astype(jnp.bfloat16)

    half = w_query.shape[1]
    gla_rows_t = w_out_gla.T
    cut = gla_rows_t.shape[1] // 2
    pairs = (
        (w_conv_a, w_conv_gate),
        (jnp.concatenate([w_query, w_key, w_decay], axis=1), w_value),
        (w_out_conv.T, w_outgate),
        (gla_rows_t[:, :cut], gla_rows_t[:, cut:]),
    )

    def held(arrays, *earlier):
        return after(arrays, *earlier) if fold else arrays

    if fold:
        along, near, far = along_z_pair, near_pair, far_pair
    else:

        def along(first, second):
            return gather(first), gather(second)

        def near(first, second):
            return first, second

        far = near

    near_2 = near(*along(*pairs[0]))
    near_1 = near(*along(*pairs[1]))
    along_3 = along(*pairs[2])
    along_4 = along(*held(pairs[3], normed))
    full_a, full_gate = far(*held(near_2, normed))
    full_qkd, full_v = far(*held(near_1, normed))
    conv_a = project(normed, full_a).astype(jnp.bfloat16)
    conv_gate = project(normed, full_gate).astype(jnp.bfloat16)
    gated = (conv_a.astype(jnp.float32) * jax.nn.sigmoid(conv_gate.astype(jnp.float32))).astype(jnp.bfloat16)
    near_3 = near(*held(along_3, gated))
    conv_out = conv_branch(gated, conv_weight, conv_gain)
    query_keys = project(normed, full_qkd[:, : 2 * half]).astype(jnp.bfloat16)
    decay_pre = project(normed, full_qkd[:, 2 * half :])
    values = project(normed, full_v).astype(jnp.bfloat16)
    out_conv = finish_x(near_3[0]) if fold else near_3[0]
    full_outgate = finish_y(near_3[1]) if fold else near_3[1]
    near_4 = near(*held(along_4, gated))
    attn, since, end, end_log = gla_local(
        query_keys[:, :half], query_keys[:, half:], values, decay_pre, decay_extra, decay_bias
    )
    packed = jnp.concatenate([end, jnp.broadcast_to(jnp.exp(end_log), (16, half))], axis=0).astype(jnp.bfloat16)
    ends = gather(packed)
    out_gla = far(*held(near_4, values))
    out_gate = project(normed, full_outgate).astype(jnp.bfloat16)
    gla_out = gla_finish(attn, since, out_gate, ends, init_state, head_gain, me, fold)

    def merged(conv_rows, gla_rows):
        total = dot(conv_rows, out_conv, ((1,), (1,))) + dot(gla_rows[:, :cut], out_gla[0], ((1,), (1,)))
        total = total + dot(gla_rows[:, cut:], out_gla[1], ((1,), (1,)))
        return total.astype(jnp.bfloat16)

    if not fold:
        return lax.psum_scatter(merged(conv_out, gla_out), "tp", scatter_dimension=0, tiled=True)
    rows = conv_out.shape[0] // 2

    def part(index):
        return merged(
            lax.dynamic_slice_in_dim(conv_out, index * rows, rows),
            lax.dynamic_slice_in_dim(gla_out, index * rows, rows),
        )

    arriving = lax.ppermute(part(1 - tp), "tp", [(0, 1), (1, 0)])
    return merge_folded(part(tp), arriving, me)


def solution(mesh):
    placed = (
        P("sp", "tp"), P(), P("sp", "tp"), P("sp", "tp"), P(None, "tp"), P("tp"), P("sp", "tp"), P("sp", "tp"),
        P("sp", "tp"), P("sp", "tp"), P("sp", "tp"), P("tp"), P("sp", "tp"), P(), P("tp", None, None),
        P("tp", "sp"), P("tp", "sp"),
    )

    def step(*arrays):
        return per_device(*arrays)

    step = jax.shard_map(
        step, mesh=mesh, in_specs=placed, out_specs=P(("sp", "tp"), None), check_vma=False
    )
    return step
```
